256 devices in a mesh: grp: 2 (over y), sp: 32 (over z, core), tp: 4 (over x).
Axes of the slice: x: 4, y: 2, z: 16, core: 2. Of those that a mesh axis runs over, the one named last changes fastest.
The devices are a block of a 4x16x16 slice.
Arguments:
- queries: bfloat16 [8192, 512], P(('grp', 'sp'), 'tp'), parts along dimension 0, may hold values from -6 to 6
- key_rows: bfloat16 [8192, 512], P(('grp', 'sp'), 'tp'), parts along dimension 0, may hold values from -6 to 6
- value_rows: bfloat16 [8192, 512], P(('grp', 'sp'), 'tp'), parts along dimension 0, may hold values from -16 to 16
- key_bias: bfloat16 [8, 8192], P('tp', ('grp', 'sp')), parts along dimension 1, may hold values from -20 to 0
- residual: bfloat16 [8192, 2048], P(('grp', 'sp')), parts along dimension 0, may hold values from -6 to 6
- out_weight: bfloat16 [512, 2048], P('tp'), may hold values from -0.25 to 0.25
- norm_gain: bfloat16 [2048], replicated, may hold values from 0.099609375 to 1.8984375
- gate_weight: bfloat16 [2048, 3072], P('sp', 'tp'), may hold values from -0.125 to 0.125
- up_weight: bfloat16 [2048, 3072], P('sp', 'tp'), may hold values from -0.125 to 0.125
- down_weight: bfloat16 [3072, 2048], P('tp', 'sp'), may hold values from -0.109375 to 0.109375
Outputs:
- layer_out: bfloat16 [8192, 2048], P(('grp', 'sp')), parts along dimension 0
The draws below stay inside these ranges and needn't reach their ends.
There are 2 independent parts, one for each index of `grp`. The reference program is written for one: setup_inputs(seed, part) draws one part's arguments, and reference() takes and returns one part's arrays. A program takes and returns all parts, laid end to end along the dimension named above; an argument that names none is the same for every part. Nothing has to cross between parts.
All inputs are finite; a program needn't handle non-finite values.
Results may differ from the reference program's by a relative error of at most 0.014.
Values may be sent and summed in bfloat16 or wider, within the bound.
No kernel may reach another device: no remote copies, remote signals or barrier semaphores. Data moves between devices by JAX's collectives and lax.ppermute only.
A program may use at most 64 MiB of HBM per device.

```python
import jax
import jax.numpy as jnp
from jax import lax

D = 2048
HEAD_TOTAL = 8
HEAD_DIM = 64
FF = 3072
TOK_DEV = 128
SEQUENCE_LENGTH = 4096
QK = 512
N_TP = 4


def draw_value_rows(key, part):
    first_key, second_key = jax.random.split(jax.random.fold_in(key, 11))
    span_len = max(TOK_DEV // 2, 1)
    n_spans = SEQUENCE_LENGTH // span_len
    offsets = 2.0 * jax.random.normal(first_key, (n_spans, 1, QK), jnp.float32)
    noise = jax.random.normal(second_key, (n_spans, span_len, QK), jnp.float32)
    return jnp.clip((offsets + noise).reshape(SEQUENCE_LENGTH, QK), -16.0, 16.0).astype(jnp.bfloat16)


def draw_key_bias(key, part):
    random_subkey_list = jax.random.split(jax.random.fold_in(key, 23), 6)
    span_len = max(TOK_DEV // 2, 1)
    n_spans = SEQUENCE_LENGTH // span_len
    share = 0.5
    fast = jax.random.uniform(random_subkey_list[0], (HEAD_TOTAL, 1, 1), jnp.float32) < share
    slow_level = -jnp.log(SEQUENCE_LENGTH * 1.0) - 1.0 + jax.random.uniform(random_subkey_list[1], (HEAD_TOTAL, 1, 1), jnp.float32, minval=-0.5, maxval=0.5)
    fast_level = -3.7 + jax.random.uniform(random_subkey_list[2], (HEAD_TOTAL, 1, 1), jnp.float32, minval=-0.5, maxval=0.5)
    level = jnp.where(fast, fast_level, slow_level)
    factor = jax.random.uniform(random_subkey_list[3], (HEAD_TOTAL, n_spans, 1), jnp.float32, minval=-0.9, maxval=0.9)
    smoothed_values = (level + factor + jnp.zeros((HEAD_TOTAL, n_spans, span_len), jnp.float32)).reshape(HEAD_TOTAL, SEQUENCE_LENGTH)
    spike_amount = jax.random.uniform(random_subkey_list[4], (HEAD_TOTAL, SEQUENCE_LENGTH), jnp.float32) < 3.0 / SEQUENCE_LENGTH
    spike_threshold = jax.random.uniform(random_subkey_list[5], (HEAD_TOTAL, SEQUENCE_LENGTH), jnp.float32, minval=-1.0, maxval=0.0)
    return jnp.where(spike_amount, spike_threshold, smoothed_values).astype(jnp.bfloat16)


def shard_levels(key, extent, cuts, least, top_value):
    def one(position, parts):
        steps = jax.random.uniform(jax.random.fold_in(jax.random.fold_in(key, 6), position), (parts,), jnp.float32, least / len(cuts), top_value / len(cuts))
        return jnp.repeat(jnp.exp(steps), extent[position] // parts).reshape((-1,) + (1,) * (len(extent) - position - 1))

    factor_of = one(*cuts[0])
    for cut in cuts[1:]:
        factor_of = factor_of * one(*cut)
    return factor_of


def gaussian(rng, shape, spread, reach, cuts=(), kind=jnp.bfloat16):
    factor_of = shard_levels(rng, shape, cuts, -0.22, 0.18) if cuts else 1.0
    drawn = jax.random.normal(rng, shape, jnp.float32) * spread * factor_of
    return jnp.minimum(jnp.maximum(drawn, -reach), reach).astype(kind)


def setup_inputs(seed: int = 0, part: int = 0) -> dict:
    key_list = jax.random.split(jax.random.key(seed), 11)
    part_keys = jax.random.split(jax.random.fold_in(key_list[10], part), 11)
    return {
        "queries": gaussian(part_keys[0], (SEQUENCE_LENGTH, QK), 1.0, 6.0, ((0, 32), (1, 4))),
        "key_rows": gaussian(part_keys[1], (SEQUENCE_LENGTH, QK), 1.0, 6.0, ((0, 32), (1, 4))),
        "value_rows": draw_value_rows(jax.random.fold_in(jax.random.fold_in(key_list[10], part), 71), part),
        "key_bias": draw_key_bias(jax.random.fold_in(jax.random.fold_in(key_list[10], part), 71), part),
        "residual": gaussian(part_keys[4], (SEQUENCE_LENGTH, D), 1.0, 6.0, ((0, 32),)),
        "out_weight": gaussian(key_list[5], (QK, D), QK ** -0.5, 0.25, ((0, 4),)),
        "norm_gain": jnp.clip(1.0 + 0.18 * jax.random.normal(key_list[6], (D,), jnp.float32), 0.099609375, 1.8984375).astype(jnp.bfloat16),
        "gate_weight": gaussian(key_list[7], (D, FF), D ** -0.5, 0.125, ((0, 32), (1, 4))),
        "up_weight": gaussian(key_list[8], (D, FF), D ** -0.5, 0.125, ((0, 32), (1, 4))),
        "down_weight": gaussian(key_list[9], (FF, D), FF ** -0.5, 0.109375, ((0, 4), (1, 32))),
    }


def stick_attention(queries, key_rows, value_rows, key_bias):
    query_heads = queries.reshape(SEQUENCE_LENGTH, HEAD_TOTAL, HEAD_DIM).astype(jnp.float32)
    key_heads = key_rows.reshape(SEQUENCE_LENGTH, HEAD_TOTAL, HEAD_DIM).astype(jnp.float32)
    value_heads = value_rows.reshape(SEQUENCE_LENGTH, HEAD_TOTAL, HEAD_DIM).astype(jnp.float32)
    bias_all = key_bias.astype(jnp.float32)
    key_pos = lax.iota(jnp.int32, SEQUENCE_LENGTH)

    def one_block(block_index):
        begin = (block_index * TOK_DEV).astype(jnp.int32)
        query_block = lax.dynamic_slice_in_dim(query_heads, begin, TOK_DEV, 0)
        scores = jnp.einsum('qhd,khd->hqk', query_block, key_heads) * HEAD_DIM ** (-0.5)
        scores = scores + bias_all[:, None, :]
        query_pos = begin + lax.iota(jnp.int32, TOK_DEV)
        strict = (key_pos[None, :] < query_pos[:, None])[None]
        log_retained = jnp.where(strict, jax.nn.log_sigmoid(-scores), 0.0)
        between = lax.cumsum(log_retained, axis=2, reverse=True) - log_retained
        stick = jnp.where(strict, jnp.exp(jax.nn.log_sigmoid(scores) + between), 0.0).astype(jnp.bfloat16)
        stick = lax.optimization_barrier(stick).astype(jnp.float32)
        return jnp.einsum('hqk,khd->qhd', stick, value_heads)
    blocks = lax.map(one_block, jnp.arange(SEQUENCE_LENGTH // TOK_DEV, dtype=jnp.int32))
    return blocks.reshape(SEQUENCE_LENGTH, QK).astype(jnp.bfloat16)

def grouped_product(left, right, groups):
    width_group = left.shape[1] // groups
    summed = jnp.zeros((left.shape[0], right.shape[1]), jnp.float32)
    for group in range(groups):
        part_prod = jnp.dot(left[:, group * width_group:(group + 1) * width_group], right[group * width_group:(group + 1) * width_group], preferred_element_type=jnp.float32).astype(jnp.bfloat16)
        summed = summed + lax.optimization_barrier(part_prod).astype(jnp.float32)
    return summed

def reference(queries, key_rows, value_rows, key_bias, residual, out_weight, norm_gain, gate_weight, up_weight, down_weight):
    attended = stick_attention(queries, key_rows, value_rows, key_bias)
    mixed = grouped_product(attended, out_weight, N_TP)
    middle = (residual.astype(jnp.float32) + mixed).astype(jnp.bfloat16)
    middle_wide = lax.optimization_barrier(middle).astype(jnp.float32)
    mean_square = lax.optimization_barrier(jnp.mean(middle_wide * middle_wide, axis=1, keepdims=True))
    normed = (middle_wide * lax.rsqrt(mean_square + 1e-05) * norm_gain.astype(jnp.float32)).astype(jnp.bfloat16)
    gate_pre = jnp.dot(normed, gate_weight, preferred_element_type=jnp.float32)
    up_pre = jnp.dot(normed, up_weight, preferred_element_type=jnp.float32)
    hidden = (jax.nn.silu(gate_pre) * up_pre).astype(jnp.bfloat16)
    down_sum = grouped_product(hidden, down_weight, N_TP)
    return (middle_wide + down_sum).astype(jnp.bfloat16)
```

```python
import functools

import jax
import jax.numpy as jnp
from jax import lax
from jax.experimental import pallas as pl
from jax.experimental.pallas import tpu as pltpu
from jax.sharding import PartitionSpec as P

norm_eps = 1e-05
f32 = jnp.float32
bf16 = jnp.bfloat16
LANES = 128


def call(kernel, outs, n_in, flops=1, scratch=(), moved=1 << 20):
    return pl.pallas_call(
        kernel,
        out_shape=[jax.ShapeDtypeStruct(s, t) for s, t in outs],
        in_specs=[pl.BlockSpec(memory_space=pltpu.SMEM)]
        + [pl.BlockSpec(memory_space=pltpu.VMEM)] * n_in,
        out_specs=[pl.BlockSpec(memory_space=pltpu.VMEM)] * len(outs),
        scratch_shapes=list(scratch),
        compiler_params=pltpu.CompilerParams(vmem_limit_bytes=56 << 20),
        cost_estimate=pl.CostEstimate(flops=flops, bytes_accessed=moved, transcendentals=0),
    )


def half(ref, side, width):
    return jnp.where(side == 0, ref[:, :width], ref[:, width:])


def split_kernel(place, q, k, v, bias, gate, up, down, own_a, send_a, own_w, send_w):
    core = place[1]
    tokens, both = q.shape
    width = both // 2
    for side, a, w in ((core, own_a, own_w), (1 - core, send_a, send_w)):
        a[:tokens, :] = jnp.concatenate([half(k, side, width), half(v, side, width)], axis=1)
        scaled = half(q, side, width).astype(f32) * width ** (-0.5)
        a[tokens : 2 * tokens, :] = jnp.concatenate(
            [scaled.astype(bf16), jnp.zeros((tokens, width), bf16)], axis=1
        )
        row = jnp.where(side == 0, bias[0:1, :], bias[1:2, :])
        a[2 * tokens :, :] = jnp.broadcast_to(row, (16, tokens))
        rows, units = gate.shape
        tiles = units // 2 // LANES
        for n, ref in enumerate((gate, up)):
            for t in range(tiles):
                lo = ref[:, t * LANES : (t + 1) * LANES]
                hi = ref[:, units // 2 + t * LANES : units // 2 + (t + 1) * LANES]
                at = (n * tiles + t) * rows
                w[at : at + rows, :] = jnp.where(side == 0, lo, hi)
        mine = pl.ds(pl.multiple_of(side * (units // 2), units // 2), units // 2)
        cut = units // 4
        piece = down[mine, :]
        w[2 * tiles * rows :, :] = jnp.concatenate([piece[:cut], piece[cut:]], axis=1)


def join_a_kernel(place, own, got, kv, q):
    core = place[1]
    tokens = own.shape[1]
    for side, ref in ((core, own), (1 - core, got)):
        rows = pl.ds(pl.multiple_of(side * tokens, tokens), tokens)
        kv[rows, :] = ref[:tokens, :]
        q[rows, :] = ref[tokens : 2 * tokens, :]
    first = jnp.where(core == 0, own[2 * tokens :, :], got[2 * tokens :, :])
    second = jnp.where(core == 0, got[2 * tokens :, :], own[2 * tokens :, :])
    line = lax.broadcasted_iota(jnp.int32, first.shape, 0)
    kv[2 * tokens :, :] = jnp.where(line == 0, first, second)


def join_w_kernel(place, own, got, wide, down, rows, tiles):
    core = place[1]
    for side, ref in ((core, own), (1 - core, got)):
        for t in range(2 * tiles):
            to = pl.ds(pl.multiple_of(t * 2 * rows + side * rows, rows), rows)
            wide[to, :] = ref[t * rows : (t + 1) * rows, :]
    cut = own.shape[0] - 2 * tiles * rows
    a = jnp.where(core == 0, own[2 * tiles * rows :, :], got[2 * tiles * rows :, :])
    b = jnp.where(core == 0, got[2 * tiles * rows :, :], own[2 * tiles * rows :, :])
    w = LANES // 2
    down[:cut, :] = jnp.concatenate([a[:, :w], b[:, :w]], axis=1)
    down[cut:, :] = jnp.concatenate([a[:, w:], b[:, w:]], axis=1)


def attend_kernel(place, q_ref, *refs):
    n = len(refs) - 4
    blocks, out, accum, carry, later = refs[:n], refs[n], refs[n + 1], refs[n + 2], refs[n + 3]
    z = place[0]
    count = q_ref.shape[0]
    shape = (count, count)
    row = lax.broadcasted_iota(jnp.int32, later.shape, 0)
    col = lax.broadcasted_iota(jnp.int32, later.shape, 1)
    later[...] = ((row > col) | (col >= count)).astype(f32).astype(bf16)
    accum[...] = jnp.zeros_like(accum)
    carry[...] = jnp.zeros_like(carry)

    def visit(block, diagonal):
        keys = block[:count, :]
        bias = jnp.concatenate(
            [block[count : count + 1, :], block[count + 1 : count + 2, :]], axis=1
        ).astype(f32)
        scores = lax.dot_general(
            q_ref[...], keys, (((1,), (1,)), ((), ())), preferred_element_type=f32
        )
        scores = scores + bias
        keep = -(jnp.maximum(scores, 0.0) + jnp.log1p(jnp.exp(-jnp.abs(scores))))
        total = scores + keep
        if diagonal:
            r = lax.broadcasted_iota(jnp.int32, shape, 0)
            c = lax.broadcasted_iota(jnp.int32, shape, 1)
            keep = jnp.where(c < r, keep, 0.0)
        high = keep.astype(bf16)
        low = (keep - high.astype(f32)).astype(bf16)
        sums = jnp.dot(high, later[...], preferred_element_type=f32) + jnp.dot(
            low, later[...], preferred_element_type=f32
        )
        before = carry[...]
        stick = jnp.exp(total + sums[:, :count] + jnp.concatenate([before, before], axis=1))
        if diagonal:
            stick = jnp.where(c < r, stick, 0.0)
        accum[...] += jnp.dot(stick.astype(bf16), keys, preferred_element_type=f32)
        carry[...] = before + sums[:, count:]

    for d, block in enumerate(blocks):
        if d == 0:
            visit(block, True)
        else:
            pl.when(z >= d)(functools.partial(visit, block, False))
    tokens = count // 2
    lane = lax.broadcasted_iota(jnp.int32, (tokens, LANES), 1)
    out[...] = jnp.where(
        lane < LANES // 2,
        pltpu.roll(accum[:tokens, :], LANES // 2, 1),
        accum[tokens:, :],
    ).astype(bf16)


def middle_kernel(place, *refs):
    n = (len(refs) - 6) // 3
    own_heads, other_heads, weights = refs[:n], refs[n : 2 * n], refs[2 * n : 3 * n]
    own_res, other_res, gain, normed, middle, scratch = refs[3 * n :]
    z, core = place[0], place[1]
    tokens = own_res.shape[0]
    width = own_res.shape[1]
    lane = lax.broadcasted_iota(jnp.int32, (tokens, LANES), 1)
    lefts = []
    for own, other in zip(own_heads, other_heads):
        a, b = own[...].astype(f32), other[...].astype(f32)
        zero = jnp.where(core == 0, a, b)
        one = jnp.where(core == 0, b, a)
        w = LANES // 2
        first = jnp.where(lane < w, zero, pltpu.roll(one, w, 1))
        second = jnp.where(lane < w, pltpu.roll(zero, w, 1), one)
        mine = jnp.where(core == 0, first, second)
        theirs = jnp.where(core == 0, second, first)
        lefts.append(jnp.concatenate([mine, theirs], axis=0).astype(bf16))
    step = 2 * LANES
    squares = jnp.zeros((2 * tokens, LANES), f32)
    for at in range(0, width, step):
        here = slice(at, at + step)
        mixed = jnp.zeros((2 * tokens, step), f32)
        for left, weight in zip(lefts, weights):
            part = jnp.dot(left, weight[:, here], preferred_element_type=f32)
            mixed = mixed + part.astype(bf16).astype(f32)
        res = jnp.concatenate([own_res[:, here], other_res[:, here]], axis=0).astype(f32)
        mid = (res + mixed).astype(bf16)
        scratch[:, here] = mid
        middle[:, here] = mid[:tokens]
        wide = mid.astype(f32)
        for b in range(0, step, LANES):
            squares = squares + wide[:, b : b + LANES] * wide[:, b : b + LANES]
    scale = lax.rsqrt(jnp.sum(squares, axis=1, keepdims=True) / width + norm_eps)
    blocks = normed.shape[0]
    for b in range(blocks):
        here = slice(b * LANES, (b + 1) * LANES)
        value = scratch[:, here].astype(f32) * scale * gain[:, here].astype(f32)
        normed[lax.rem(z - b + blocks, blocks)] = value.astype(bf16)


def feed_kernel(place, normed, *refs):
    blocks = normed.shape[0]
    wides, downs = refs[:blocks], refs[blocks : 2 * blocks]
    own, other = refs[2 * blocks :]
    z = place[0]
    rows = LANES
    tiles = wides[0].shape[0] // rows // 2
    tokens = own.shape[0]
    hidden = []
    for t in range(tiles):
        both = None
        for d in range(0, blocks, 2):
            left = jnp.concatenate([normed[d], normed[d + 1]], axis=1)
            right = jnp.concatenate(
                [
                    jnp.concatenate(
                        [
                            w[t * rows : (t + 1) * rows, :],
                            w[(tiles + t) * rows : (tiles + t + 1) * rows, :],
                        ],
                        axis=1,
                    )
                    for w in (wides[d], wides[d + 1])
                ],
                axis=0,
            )
            part = jnp.dot(left, right, preferred_element_type=f32)
            both = part if both is None else both + part
        gate, up = both[:, :LANES], both[:, LANES:]
        hidden.append((gate / (1.0 + jnp.exp(-gate)) * up).astype(bf16))
    hidden = jnp.concatenate(hidden, axis=1)
    for d in range(0, blocks, 2):
        right = jnp.concatenate([downs[d][...], downs[d + 1][...]], axis=1)
        part = jnp.dot(hidden, right, preferred_element_type=f32)
        for e in range(2):
            column = lax.rem(z - (d + e) + blocks, blocks)
            here = pl.ds(pl.multiple_of(column * LANES, LANES), LANES)
            own[:, here] = part[:tokens, e * LANES : (e + 1) * LANES]
            other[:, here] = part[tokens:, e * LANES : (e + 1) * LANES].astype(bf16)


def pair_kernel(place, own, got, *sends):
    me = place[2]
    rows = sends[0].shape[0]
    for k, send in enumerate(sends):
        here = pl.ds(pl.multiple_of(lax.bitwise_xor(me, k) * rows, rows), rows)
        send[...] = (own[here, :] + got[here, :].astype(f32)).astype(bf16)


def owner_kernel(place, middle, *refs):
    parts, out = refs[:-1], refs[-1]
    rows = out.shape[0]
    here = pl.ds(pl.multiple_of(place[2] * rows, rows), rows)
    summed = parts[0][...].astype(f32)
    for part in parts[1:]:
        summed = summed + part[...].astype(f32)
    out[...] = (middle[here, :].astype(f32) + summed).astype(bf16)


def order_kernel(place, *refs):
    parts, out = refs[:-1], refs[-1]
    rows = parts[0].shape[0]
    for k, part in enumerate(parts):
        out[pl.ds(pl.multiple_of(lax.bitwise_xor(place[2], k) * rows, rows), rows), :] = part[...]


def swap(value):
    n = lax.axis_size("sp")
    return lax.ppermute(value, "sp", [(i, i ^ 1) for i in range(n)])


def across(value, k):
    n = lax.axis_size("tp")
    return lax.ppermute(value, "tp", [(i, i ^ k) for i in range(n)])


def hop(value, step):
    n = lax.axis_size("sp")
    return lax.ppermute(value, "sp", [(i, (i + 2 * step) % n) for i in range(n)])


def ring(block):
    n = lax.axis_size("sp") // 2
    out = [None] * n
    out[0] = block
    right = left = block
    for s in range(1, n // 2 + 1):
        right = hop(right, 1)
        out[s] = right
        if s < n - s:
            left = hop(left, -1)
            out[n - s] = left
    return out


def body(
    queries,
    key_rows,
    value_rows,
    key_bias,
    residual,
    out_weight,
    norm_gain,
    gate_weight,
    up_weight,
    down_weight,
):
    tokens, model = residual.shape
    rows, units = gate_weight.shape
    chips = lax.axis_size("sp") // 2
    n_tp = lax.axis_size("tp")
    tiles = units // 2 // LANES
    here = lax.axis_index("sp")
    place = jnp.stack([here // 2, here % 2, lax.axis_index("tp")]).astype(jnp.int32)

    a_shape = (2 * tokens + 16, LANES)
    w_shape = (2 * tiles * rows + units // 4, LANES)
    own_a, send_a, own_w, send_w = call(
        split_kernel, [(a_shape, bf16), (a_shape, bf16), (w_shape, bf16), (w_shape, bf16)], 7
    )(place, queries, key_rows, value_rows, key_bias, gate_weight, up_weight, down_weight)
    got_a = swap(send_a)
    got_w = swap(send_w)
    kv, q = call(join_a_kernel, [(a_shape, bf16), ((2 * tokens, LANES), bf16)], 2)(
        place, own_a, got_a
    )
    wide, down = call(
        functools.partial(join_w_kernel, rows=rows, tiles=tiles),
        [((4 * tiles * rows, LANES), bf16), ((units // 2, LANES), bf16)],
        2,
    )(place, own_w, got_w)

    kv_blocks = ring(kv)
    wide_blocks = ring(wide)
    down_blocks = ring(down)
    other_res = swap(residual)
    weights = [out_weight] + [across(out_weight, k) for k in range(1, n_tp)]

    count = 2 * tokens
    heads = call(
        attend_kernel,
        [((tokens, LANES), bf16)],
        1 + chips,
        flops=10 * count * count * chips * LANES,
        scratch=[
            pltpu.VMEM((count, LANES), f32),
            pltpu.VMEM((count, LANES), f32),
            pltpu.VMEM((count, count + LANES), bf16),
        ],
    )(place, q, *kv_blocks)[0]
    own_heads = [heads] + [across(heads, k) for k in range(1, n_tp)]
    other_heads = [swap(h) for h in own_heads]
    normed, middle = call(
        middle_kernel,
        [((model // LANES, count, LANES), bf16), ((tokens, model), bf16)],
        3 * n_tp + 3,
        flops=2 * count * n_tp * LANES * model,
        scratch=[pltpu.VMEM((count, model), bf16)],
    )(place, *own_heads, *other_heads, *weights, residual, other_res, norm_gain.reshape(1, -1))
    own, other = call(
        feed_kernel,
        [((tokens, model), f32), ((tokens, model), bf16)],
        1 + 2 * chips,
        flops=6 * count * model * units // 2,
    )(place, normed, *wide_blocks, *down_blocks)
    got = swap(other)
    share = (tokens // n_tp, model)
    sends = call(pair_kernel, [(share, bf16)] * n_tp, 2)(place, own, got)
    parts = [sends[0]] + [across(sends[k], k) for k in range(1, n_tp)]
    mine = call(owner_kernel, [(share, bf16)], 1 + n_tp)(place, middle, *parts)[0]
    all_rows = [mine] + [across(mine, k) for k in range(1, n_tp)]
    return call(order_kernel, [((tokens, model), bf16)], n_tp)(place, *all_rows)[0]


def solution(mesh):
    in_specs = (
        P(("grp", "sp"), "tp"),
        P(("grp", "sp"), "tp"),
        P(("grp", "sp"), "tp"),
        P("tp", ("grp", "sp")),
        P(("grp", "sp"), None),
        P("tp", None),
        P(),
        P("sp", "tp"),
        P("sp", "tp"),
        P("tp", "sp"),
    )
    out_specs = P(("grp", "sp"), None)
    return jax.shard_map(body, mesh=mesh, in_specs=in_specs, out_specs=out_specs, check_vma=False)
```

```python
import functools

import jax
import jax.numpy as jnp
from jax import lax
from jax.experimental import pallas as pl
from jax.experimental.pallas import tpu as pltpu
from jax.sharding import PartitionSpec as P

norm_eps = 1e-05
f32 = jnp.float32
bf16 = jnp.bfloat16
LANES = 128


def call(kernel, outs, n_in, flops=1, scratch=(), moved=1 << 20, n_any=0, grant=16):
    return pl.pallas_call(
        kernel,
        out_shape=[jax.ShapeDtypeStruct(s, t) for s, t in outs],
        in_specs=[pl.BlockSpec(memory_space=pltpu.SMEM)]
        + [pl.BlockSpec(memory_space=pltpu.VMEM)] * n_in
        + [pl.BlockSpec(memory_space=pl.ANY)] * n_any,
        out_specs=[pl.BlockSpec(memory_space=pltpu.VMEM)] * len(outs),
        scratch_shapes=list(scratch),
        compiler_params=pltpu.CompilerParams(vmem_limit_bytes=grant << 20),
        cost_estimate=pl.CostEstimate(flops=flops, bytes_accessed=moved, transcendentals=0),
    )


def half(ref, side, width):
    return jnp.where(side == 0, ref[:, :width], ref[:, width:])


def split_kernel(place, q, k, v, bias, own_a, send_a):
    core = place[1]
    tokens, both = q.shape
    width = both // 2
    for side, a in ((core, own_a), (1 - core, send_a)):
        a[:tokens, :] = jnp.concatenate([half(k, side, width), half(v, side, width)], axis=1)
        scaled = half(q, side, width).astype(f32) * width ** (-0.5)
        a[tokens : 2 * tokens, :] = jnp.concatenate(
            [scaled.astype(bf16), jnp.zeros((tokens, width), bf16)], axis=1
        )
        row = jnp.where(side == 0, bias[0:1, :], bias[1:2, :])
        a[2 * tokens :, :] = jnp.broadcast_to(row, (16, tokens))


def join_kernel(place, own, got, kv, q):
    core = place[1]
    tokens = own.shape[1]
    for side, ref in ((core, own), (1 - core, got)):
        rows = pl.ds(pl.multiple_of(side * tokens, tokens), tokens)
        kv[rows, :] = ref[:tokens, :]
        q[rows, :] = ref[tokens : 2 * tokens, :]
    first = jnp.where(core == 0, own[2 * tokens :, :], got[2 * tokens :, :])
    second = jnp.where(core == 0, got[2 * tokens :, :], own[2 * tokens :, :])
    line = lax.broadcasted_iota(jnp.int32, first.shape, 0)
    kv[2 * tokens :, :] = jnp.where(line == 0, first, second)


def attend_kernel(place, q_ref, *refs):
    n = len(refs) - 6
    blocks, (own, send, stack, accum, carry, later) = refs[:n], refs[n:]
    z, core = place[0], place[1]
    count = q_ref.shape[0]
    shape = (count, count)
    row = lax.broadcasted_iota(jnp.int32, later.shape, 0)
    col = lax.broadcasted_iota(jnp.int32, later.shape, 1)
    later[...] = jnp.where((row > col) | (col >= count), -1.0, 0.0).astype(bf16)
    for d, block in enumerate(blocks):
        stack[d] = block[...]

    def visit(d, before, diagonal):
        keys = stack[d, :count, :]
        bias = jnp.concatenate(
            [stack[d, count : count + 1, :], stack[d, count + 1 : count + 2, :]], axis=1
        ).astype(f32)
        bias = jnp.where(d <= z, bias, -1e30)
        scores = bias + lax.dot_general(
            q_ref[...], keys, (((1,), (1,)), ((), ())), preferred_element_type=f32
        )
        lost = jnp.maximum(scores, 0.0) + jnp.log(1.0 + jnp.exp(-jnp.abs(scores)))
        total = scores - lost
        if diagonal:
            r = lax.broadcasted_iota(jnp.int32, shape, 0)
            c = lax.broadcasted_iota(jnp.int32, shape, 1)
            lost = jnp.where(c < r, lost, 0.0)
        high = lost.astype(bf16)
        low = (lost - high.astype(f32)).astype(bf16)
        sums = jnp.dot(high, later[...], preferred_element_type=f32) + jnp.dot(
            low, later[...], preferred_element_type=f32
        )
        stick = jnp.exp(total + sums[:, :count] + jnp.concatenate([before, before], axis=1))
        if diagonal:
            stick = jnp.where(c < r, stick, 0.0)
        part = jnp.dot(stick.astype(bf16), keys, preferred_element_type=f32)
        return part, before + sums[:, count:]

    def pair(d, before, diagonal):
        first, before = visit(d, before, diagonal)
        second, before = visit(d + 1, before, False)
        return first + second, before

    part, after = pair(0, jnp.zeros(carry.shape, f32), True)
    accum[...] = part
    carry[...] = after

    @pl.loop(1, z // 2 + 1)
    def _(i):
        part, after = pair(2 * i, carry[...], False)
        accum[...] += part
        carry[...] = after

    tokens = count // 2
    for side, out in ((core, own), (1 - core, send)):
        rows = pl.ds(pl.multiple_of(side * tokens, tokens), tokens)
        out[...] = accum[rows, :].astype(bf16)


def heads_kernel(place, own, got, out):
    core = place[1]
    a, b = own[...].astype(f32), got[...].astype(f32)
    zero = jnp.where(core == 0, a, b)
    one = jnp.where(core == 0, b, a)
    lane = lax.broadcasted_iota(jnp.int32, out.shape, 1)
    w = LANES // 2
    out[...] = jnp.where(lane < w, pltpu.roll(zero, w, 1), one).astype(bf16)


def middle_kernel(place, *refs):
    n = (len(refs) - 5) // 2
    heads, weights = refs[:n], refs[n : 2 * n]
    residual, gain, normed, middle, scratch = refs[2 * n :]
    tokens, width = residual.shape
    rows = middle.shape[0]
    step = 2 * LANES
    squares = jnp.zeros((tokens, LANES), f32)
    for at in range(0, width, step):
        here = slice(at, at + step)
        mixed = jnp.zeros((tokens, step), f32)
        for head, weight in zip(heads, weights):
            part = jnp.dot(head[...], weight[:, here], preferred_element_type=f32)
            mixed = mixed + part.astype(bf16).astype(f32)
        mid = (residual[:, here].astype(f32) + mixed).astype(bf16)
        scratch[:, here] = mid
        wide = mid.astype(f32)
        for b in range(0, step, LANES):
            squares = squares + wide[:, b : b + LANES] * wide[:, b : b + LANES]
    scale = lax.rsqrt(jnp.sum(squares, axis=1, keepdims=True) / width + norm_eps)
    for at in range(0, width, step):
        here = slice(at, at + step)
        value = scratch[:, here].astype(f32) * scale * gain[:, here].astype(f32)
        normed[:, here] = value.astype(bf16)
    middle[...] = scratch[pl.ds(pl.multiple_of(place[2] * rows, rows), rows), :]


def feed_kernel(place, normed, weights, *refs):
    n = len(refs) - 6
    sends, (held, both, hidden, partial, wide_sem, down_sem) = refs[:n], refs[n:]
    members, rows, units = held.shape[0], held.shape[1] // 3, held.shape[2]
    chunks = wide_sem.shape[0]
    group = members // chunks
    tokens = normed.shape[0]
    depth = group * rows

    def wide_copy(c):
        part = (pl.ds(c * group, group), pl.ds(0, 2 * rows))
        return pltpu.make_async_copy(weights.at[part], held.at[part], wide_sem.at[c])

    def down_copy(c):
        part = (pl.ds(c * group, group), pl.ds(2 * rows, rows))
        return pltpu.make_async_copy(weights.at[part], held.at[part], down_sem.at[c])

    for c in range(chunks):
        wide_copy(c).start()
    for c in range(chunks):
        down_copy(c).start()
    both[...] = jnp.zeros_like(both)

    @pl.loop(0, chunks)
    def _(c):
        wide_copy(c).wait()
        left = normed[:, pl.ds(pl.multiple_of(c * depth, depth), depth)]
        some = pl.ds(c * group, group)
        for kind in range(2):
            right = held[some, kind * rows : (kind + 1) * rows, :].reshape(depth, units)
            both[:, kind * units : (kind + 1) * units] += jnp.dot(
                left, right, preferred_element_type=f32
            )

    gate, up = both[:, :units], both[:, units:]
    hidden[...] = (gate / (1.0 + jnp.exp(-gate)) * up).astype(bf16)

    @pl.loop(0, chunks)
    def _(c):
        down_copy(c).wait()
        right = held[pl.ds(c * group, group), 2 * rows :, :].reshape(depth, units)
        part = lax.dot_general(
            hidden[...], right, (((1,), (1,)), ((), ())), preferred_element_type=f32
        )
        partial[:, pl.ds(pl.multiple_of(c * depth, depth), depth)] = part.astype(bf16)

    share = sends[0].shape[0]
    for k, send in enumerate(sends):
        at = pl.multiple_of(lax.bitwise_xor(place[2], k) * share, share)
        send[...] = partial[pl.ds(at, share), :]


def owner_kernel(place, middle, *refs):
    parts, out = refs[:-1], refs[-1]
    summed = parts[0][...].astype(f32)
    for part in parts[1:]:
        summed = summed + part[...].astype(f32)
    out[...] = (middle[...].astype(f32) + summed).astype(bf16)


def order_kernel(place, *refs):
    parts, out = refs[:-1], refs[-1]
    rows = parts[0].shape[0]
    for k, part in enumerate(parts):
        out[pl.ds(pl.multiple_of(lax.bitwise_xor(place[2], k) * rows, rows), rows), :] = part[...]


def swap(value):
    n = lax.axis_size("sp")
    return lax.ppermute(value, "sp", [(i, i ^ 1) for i in range(n)])


def across(value, k):
    n = lax.axis_size("tp")
    return lax.ppermute(value, "tp", [(i, i ^ k) for i in range(n)])


def hop(value, step):
    n = lax.axis_size("sp")
    return lax.ppermute(value, "sp", [(i, (i + 2 * step) % n) for i in range(n)])


def ring(block):
    n = lax.axis_size("sp") // 2
    out = [None] * n
    out[0] = block
    right = left = block
    for s in range(1, n // 2 + 1):
        right = hop(right, 1)
        out[s] = right
        if s < n - s:
            left = hop(left, -1)
            out[n - s] = left
    return out


def body(
    queries,
    key_rows,
    value_rows,
    key_bias,
    residual,
    out_weight,
    norm_gain,
    gate_weight,
    up_weight,
    down_weight,
):
    tokens, model = residual.shape
    rows, units = gate_weight.shape
    members = lax.axis_size("sp")
    chips = members // 2
    n_tp = lax.axis_size("tp")
    here = lax.axis_index("sp")

    packed = jnp.concatenate([gate_weight, up_weight, down_weight.T], axis=0)
    gathered = lax.all_gather(packed, "sp", axis=0, tiled=False)

    place = jnp.stack([here // 2, here % 2, lax.axis_index("tp")]).astype(jnp.int32)
    a_shape = (2 * tokens + 16, LANES)
    own_a, send_a = call(split_kernel, [(a_shape, bf16), (a_shape, bf16)], 4)(
        place, queries, key_rows, value_rows, key_bias
    )
    count = 2 * tokens
    kv, q = call(join_kernel, [(a_shape, bf16), ((count, LANES), bf16)], 2)(
        place, own_a, swap(send_a)
    )
    kv_blocks = ring(kv)
    weights = [out_weight] + [across(out_weight, k) for k in range(1, n_tp)]

    half_heads, send_heads = call(
        attend_kernel,
        [((tokens, LANES), bf16)] * 2,
        1 + chips,
        flops=10 * count * count * chips * LANES,
        scratch=[
            pltpu.VMEM((chips, count + 16, LANES), bf16),
            pltpu.VMEM((count, LANES), f32),
            pltpu.VMEM((count, LANES), f32),
            pltpu.VMEM((count, count + LANES), bf16),
        ],
    )(place, q, *kv_blocks)
    heads = call(heads_kernel, [((tokens, LANES), bf16)], 2)(place, half_heads, swap(send_heads))[0]
    all_heads = [heads] + [across(heads, k) for k in range(1, n_tp)]
    share = (tokens // n_tp, model)
    normed, middle = call(
        middle_kernel,
        [((tokens, model), bf16), (share, bf16)],
        2 * n_tp + 2,
        flops=2 * tokens * n_tp * LANES * model,
        scratch=[pltpu.VMEM((tokens, model), bf16)],
    )(place, *all_heads, *weights, residual, norm_gain.reshape(1, -1))
    chunks = 4
    sends = call(
        feed_kernel,
        [(share, bf16)] * n_tp,
        1,
        n_any=1,
        grant=56,
        flops=6 * tokens * model * units,
        scratch=[
            pltpu.VMEM((members, 3 * rows, units), bf16),
            pltpu.VMEM((tokens, 2 * units), f32),
            pltpu.VMEM((tokens, units), bf16),
            pltpu.VMEM((tokens, model), bf16),
            pltpu.SemaphoreType.DMA((chunks,)),
            pltpu.SemaphoreType.DMA((chunks,)),
        ],
    )(place, normed, gathered)
    parts = [sends[0]] + [across(sends[k], k) for k in range(1, n_tp)]
    mine = call(owner_kernel, [(share, bf16)], 1 + n_tp)(place, middle, *parts)[0]
    all_rows = [mine] + [across(mine, k) for k in range(1, n_tp)]
    return call(order_kernel, [((tokens, model), bf16)], n_tp)(place, *all_rows)[0]


def solution(mesh):
    in_specs = (
        P(("grp", "sp"), "tp"),
        P(("grp", "sp"), "tp"),
        P(("grp", "sp"), "tp"),
        P("tp", ("grp", "sp")),
        P(("grp", "sp"), None),
        P("tp", None),
        P(),
        P("sp", "tp"),
        P("sp", "tp"),
        P("tp", "sp"),
    )
    out_specs = P(("grp", "sp"), None)
    return jax.shard_map(body, mesh=mesh, in_specs=in_specs, out_specs=out_specs, check_vma=False)
```

```python
import functools

import jax
import jax.numpy as jnp
from jax import lax
from jax.experimental import pallas as pl
from jax.experimental.pallas import tpu as pltpu
from jax.sharding import PartitionSpec as P

norm_eps = 1e-05
f32 = jnp.float32
bf16 = jnp.bfloat16
LANES = 128


def call(kernel, outs, n_in, flops=1, scratch=(), moved=1 << 20, n_any=0, grant=16):
    return pl.pallas_call(
        kernel,
        out_shape=[jax.ShapeDtypeStruct(s, t) for s, t in outs],
        in_specs=[pl.BlockSpec(memory_space=pltpu.SMEM)]
        + [pl.BlockSpec(memory_space=pltpu.VMEM)] * n_in
        + [pl.BlockSpec(memory_space=pl.ANY)] * n_any,
        out_specs=[pl.BlockSpec(memory_space=pltpu.VMEM)] * len(outs),
        scratch_shapes=list(scratch),
        compiler_params=pltpu.CompilerParams(vmem_limit_bytes=grant << 20),
        cost_estimate=pl.CostEstimate(flops=flops, bytes_accessed=moved, transcendentals=0),
    )


def half(ref, side, width):
    return jnp.where(side == 0, ref[:, :width], ref[:, width:])


def split_kernel(place, packed, own_a, send_a):
    core = place[1]
    tokens, both = (packed.shape[0] - 16) // 3, packed.shape[1]
    q, k, v = (packed.at[n * tokens : (n + 1) * tokens] for n in range(3))
    bias = packed.at[3 * tokens :]
    width = both // 2
    for side, a in ((core, own_a), (1 - core, send_a)):
        a[:tokens, :] = jnp.concatenate([half(k, side, width), half(v, side, width)], axis=1)
        scaled = half(q, side, width).astype(f32) * width ** (-0.5)
        a[tokens : 2 * tokens, :] = jnp.concatenate(
            [scaled.astype(bf16), jnp.zeros((tokens, width), bf16)], axis=1
        )
        row = jnp.where(side == 0, bias[0:1, :], bias[1:2, :])
        a[2 * tokens :, :] = jnp.broadcast_to(row, (16, tokens))


def join_kernel(place, own, got, kv, q):
    core = place[1]
    tokens = own.shape[1]
    for side, ref in ((core, own), (1 - core, got)):
        rows = pl.ds(pl.multiple_of(side * tokens, tokens), tokens)
        kv[rows, :] = ref[:tokens, :]
        q[rows, :] = ref[tokens : 2 * tokens, :]
    first = jnp.where(core == 0, own[2 * tokens :, :], got[2 * tokens :, :])
    second = jnp.where(core == 0, got[2 * tokens :, :], own[2 * tokens :, :])
    line = lax.broadcasted_iota(jnp.int32, first.shape, 0)
    kv[2 * tokens :, :] = jnp.where(line == 0, first, second)


def attend_kernel(place, q_ref, *refs):
    n = len(refs) - 6
    blocks, (own, send, stack, accum, carry, later) = refs[:n], refs[n:]
    z, core = place[0], place[1]
    count = q_ref.shape[0]
    shape = (count, count)
    row = lax.broadcasted_iota(jnp.int32, later.shape, 0)
    col = lax.broadcasted_iota(jnp.int32, later.shape, 1)
    later[...] = jnp.where((row > col) | (col >= count), -1.0, 0.0).astype(bf16)
    for d, block in enumerate(blocks):
        stack[d] = block[...]

    def visit(d, before, diagonal):
        keys = stack[d, :count, :]
        bias = jnp.concatenate(
            [stack[d, count : count + 1, :], stack[d, count + 1 : count + 2, :]], axis=1
        ).astype(f32)
        bias = jnp.where(d <= z, bias, -1e30)
        scores = bias + lax.dot_general(
            q_ref[...], keys, (((1,), (1,)), ((), ())), preferred_element_type=f32
        )
        lost = jnp.maximum(scores, 0.0) + jnp.log(1.0 + jnp.exp(-jnp.abs(scores)))
        total = scores - lost
        if diagonal:
            r = lax.broadcasted_iota(jnp.int32, shape, 0)
            c = lax.broadcasted_iota(jnp.int32, shape, 1)
            lost = jnp.where(c < r, lost, 0.0)
        high = lost.astype(bf16)
        low = (lost - high.astype(f32)).astype(bf16)
        sums = jnp.dot(high, later[...], preferred_element_type=f32) + jnp.dot(
            low, later[...], preferred_element_type=f32
        )
        stick = jnp.exp(total + sums[:, :count] + jnp.concatenate([before, before], axis=1))
        if diagonal:
            stick = jnp.where(c < r, stick, 0.0)
        part = jnp.dot(stick.astype(bf16), keys, preferred_element_type=f32)
        return part, before + sums[:, count:]

    def pair(d, before, diagonal):
        first, before = visit(d, before, diagonal)
        second, before = visit(d + 1, before, False)
        return first + second, before

    part, after = pair(0, jnp.zeros(carry.shape, f32), True)
    accum[...] = part
    carry[...] = after

    @pl.loop(1, z // 2 + 1)
    def _(i):
        part, after = pair(2 * i, carry[...], False)
        accum[...] += part
        carry[...] = after

    tokens = count // 2
    for side, out in ((core, own), (1 - core, send)):
        rows = pl.ds(pl.multiple_of(side * tokens, tokens), tokens)
        out[...] = accum[rows, :].astype(bf16)


def heads_kernel(place, own, got, out):
    core = place[1]
    a, b = own[...].astype(f32), got[...].astype(f32)
    zero = jnp.where(core == 0, a, b)
    one = jnp.where(core == 0, b, a)
    lane = lax.broadcasted_iota(jnp.int32, out.shape, 1)
    w = LANES // 2
    out[...] = jnp.where(lane < w, pltpu.roll(zero, w, 1), one).astype(bf16)


def middle_kernel(place, *refs):
    n = (len(refs) - 5) // 2
    heads, weights = refs[:n], refs[n : 2 * n]
    residual, gain, normed, middle, scratch = refs[2 * n :]
    tokens, width = residual.shape
    rows = middle.shape[0]
    step = 2 * LANES
    squares = jnp.zeros((tokens, LANES), f32)
    for at in range(0, width, step):
        here = slice(at, at + step)
        mixed = jnp.zeros((tokens, step), f32)
        for head, weight in zip(heads, weights):
            part = jnp.dot(head[...], weight[:, here], preferred_element_type=f32)
            mixed = mixed + part.astype(bf16).astype(f32)
        mid = (residual[:, here].astype(f32) + mixed).astype(bf16)
        scratch[:, here] = mid
        wide = mid.astype(f32)
        for b in range(0, step, LANES):
            squares = squares + wide[:, b : b + LANES] * wide[:, b : b + LANES]
    scale = lax.rsqrt(jnp.sum(squares, axis=1, keepdims=True) / width + norm_eps)
    for at in range(0, width, step):
        here = slice(at, at + step)
        value = scratch[:, here].astype(f32) * scale * gain[:, here].astype(f32)
        normed[:, here] = value.astype(bf16)
    middle[...] = scratch[pl.ds(pl.multiple_of(place[2] * rows, rows), rows), :]


def feed_kernel(place, normed, weights, *refs):
    n = len(refs) - 6
    sends, (held, both, hidden, partial, wide_sem, down_sem) = refs[:n], refs[n:]
    members, rows, units = held.shape[0], held.shape[1] // 3, held.shape[2]
    chunks = wide_sem.shape[0]
    group = members // chunks
    tokens = normed.shape[0]
    depth = group * rows

    def wide_copy(c):
        part = (pl.ds(c * group, group), pl.ds(0, 2 * rows))
        return pltpu.make_async_copy(weights.at[part], held.at[part], wide_sem.at[c])

    def down_copy(c):
        part = (pl.ds(c * group, group), pl.ds(2 * rows, rows))
        return pltpu.make_async_copy(weights.at[part], held.at[part], down_sem.at[c])

    for c in range(chunks):
        wide_copy(c).start()
    for c in range(chunks):
        down_copy(c).start()
    both[...] = jnp.zeros_like(both)

    @pl.loop(0, chunks)
    def _(c):
        wide_copy(c).wait()
        left = normed[:, pl.ds(pl.multiple_of(c * depth, depth), depth)]
        some = pl.ds(c * group, group)
        for kind in range(2):
            right = held[some, kind * rows : (kind + 1) * rows, :].reshape(depth, units)
            both[:, kind * units : (kind + 1) * units] += jnp.dot(
                left, right, preferred_element_type=f32
            )

    gate, up = both[:, :units], both[:, units:]
    hidden[...] = (gate / (1.0 + jnp.exp(-gate)) * up).astype(bf16)

    @pl.loop(0, chunks)
    def _(c):
        down_copy(c).wait()
        right = held[pl.ds(c * group, group), 2 * rows :, :].reshape(depth, units)
        part = lax.dot_general(
            hidden[...], right, (((1,), (1,)), ((), ())), preferred_element_type=f32
        )
        partial[:, pl.ds(pl.multiple_of(c * depth, depth), depth)] = part.astype(bf16)

    share = sends[0].shape[0]
    for k, send in enumerate(sends):
        at = pl.multiple_of(lax.bitwise_xor(place[2], k) * share, share)
        send[...] = partial[pl.ds(at, share), :]


def owner_kernel(place, middle, *refs):
    parts, out = refs[:-1], refs[-1]
    summed = parts[0][...].astype(f32)
    for part in parts[1:]:
        summed = summed + part[...].astype(f32)
    out[...] = (middle[...].astype(f32) + summed).astype(bf16)


def order_kernel(place, *refs):
    parts, out = refs[:-1], refs[-1]
    rows = parts[0].shape[0]
    for k, part in enumerate(parts):
        out[pl.ds(pl.multiple_of(lax.bitwise_xor(place[2], k) * rows, rows), rows), :] = part[...]


def swap(value):
    n = lax.axis_size("sp")
    return lax.ppermute(value, "sp", [(i, i ^ 1) for i in range(n)])


def across(value, k):
    n = lax.axis_size("tp")
    return lax.ppermute(value, "tp", [(i, i ^ k) for i in range(n)])


def hop(value, step):
    n = lax.axis_size("sp")
    return lax.ppermute(value, "sp", [(i, (i + 2 * step) % n) for i in range(n)])


def ring(block):
    n = lax.axis_size("sp") // 2
    out = [None] * n
    out[0] = block
    right = left = block
    for s in range(1, n // 2 + 1):
        right = hop(right, 1)
        out[s] = right
        if s < n - s:
            left = hop(left, -1)
            out[n - s] = left
    return out


def body(
    queries,
    key_rows,
    value_rows,
    key_bias,
    residual,
    out_weight,
    norm_gain,
    gate_weight,
    up_weight,
    down_weight,
):
    tokens, model = residual.shape
    rows, units = gate_weight.shape
    members = lax.axis_size("sp")
    chips = members // 2
    n_tp = lax.axis_size("tp")
    here = lax.axis_index("sp")

    packed = jnp.concatenate([gate_weight, up_weight, down_weight.T], axis=0)
    gathered = lax.all_gather(packed, "sp", axis=0, tiled=False)

    place = jnp.stack([here // 2, here % 2, lax.axis_index("tp")]).astype(jnp.int32)
    a_shape = (2 * tokens + 16, LANES)
    bias_rows = jnp.pad(key_bias, ((0, 16 - key_bias.shape[0]), (0, 0)))
    sources = jnp.concatenate([queries, key_rows, value_rows, bias_rows], axis=0)
    own_a, send_a = call(split_kernel, [(a_shape, bf16), (a_shape, bf16)], 1)(place, sources)
    count = 2 * tokens
    kv, q = call(join_kernel, [(a_shape, bf16), ((count, LANES), bf16)], 2)(
        place, own_a, swap(send_a)
    )
    kv_blocks = ring(kv)
    weights = [out_weight] + [across(out_weight, k) for k in range(1, n_tp)]

    half_heads, send_heads = call(
        attend_kernel,
        [((tokens, LANES), bf16)] * 2,
        1 + chips,
        flops=10 * count * count * chips * LANES,
        scratch=[
            pltpu.VMEM((chips, count + 16, LANES), bf16),
            pltpu.VMEM((count, LANES), f32),
            pltpu.VMEM((count, LANES), f32),
            pltpu.VMEM((count, count + LANES), bf16),
        ],
    )(place, q, *kv_blocks)
    heads = call(heads_kernel, [((tokens, LANES), bf16)], 2)(place, half_heads, swap(send_heads))[0]
    all_heads = [heads] + [across(heads, k) for k in range(1, n_tp)]
    share = (tokens // n_tp, model)
    normed, middle = call(
        middle_kernel,
        [((tokens, model), bf16), (share, bf16)],
        2 * n_tp + 2,
        flops=2 * tokens * n_tp * LANES * model,
        scratch=[pltpu.VMEM((tokens, model), bf16)],
    )(place, *all_heads, *weights, residual, norm_gain.reshape(1, -1))
    chunks = 4
    sends = call(
        feed_kernel,
        [(share, bf16)] * n_tp,
        1,
        n_any=1,
        grant=51,
        flops=6 * tokens * model * units,
        scratch=[
            pltpu.VMEM((members, 3 * rows, units), bf16),
            pltpu.VMEM((tokens, 2 * units), f32),
            pltpu.VMEM((tokens, units), bf16),
            pltpu.VMEM((tokens, model), bf16),
            pltpu.SemaphoreType.DMA((chunks,)),
            pltpu.SemaphoreType.DMA((chunks,)),
        ],
    )(place, normed, gathered)
    parts = [sends[0]] + [across(sends[k], k) for k in range(1, n_tp)]
    mine = call(owner_kernel, [(share, bf16)], 1 + n_tp)(place, middle, *parts)[0]
    all_rows = [mine] + [across(mine, k) for k in range(1, n_tp)]
    return call(order_kernel, [((tokens, model), bf16)], n_tp)(place, *all_rows)[0]


def solution(mesh):
    in_specs = (
        P(("grp", "sp"), "tp"),
        P(("grp", "sp"), "tp"),
        P(("grp", "sp"), "tp"),
        P("tp", ("grp", "sp")),
        P(("grp", "sp"), None),
        P("tp", None),
        P(),
        P("sp", "tp"),
        P("sp", "tp"),
        P("tp", "sp"),
    )
    out_specs = P(("grp", "sp"), None)
    return jax.shard_map(body, mesh=mesh, in_specs=in_specs, out_specs=out_specs, check_vma=False)
```
